32 devices in a mesh: ep: 8 (over z, core), tp: 4 (over y, x).
Axes of the slice: x: 2, y: 2, z: 4, core: 2. Of those that a mesh axis runs over, the one named last changes fastest.
Arguments:
- query_in: bfloat16 [1024, 8192], P('tp', 'ep'), may hold values from -6 to 6
- key_in: bfloat16 [1024, 8192], P('tp', 'ep'), may hold values from -10 to 10
- value_in: bfloat16 [1024, 8192], P('tp', 'ep'), may hold values from -6 to 6
- erase_pre: bfloat16 [1024, 8192], P('tp', 'ep'), may hold values from -8 to 5
- decay_pre: bfloat16 [1024, 8192], P('tp', 'ep'), may hold values from -30 to 4.5
- mix_gain: float32 [1024], P('tp'), may hold values from 0.1 to 1.9
- expert_in: bfloat16 [2048, 2048], P('ep'), may hold values from -6 to 6
- expert_gain: float32 [2048], replicated, may hold values from 0.1 to 1.9
- routes: int32 [2048, 2], P('ep'), may hold values from 0 to 7, all different within a row; in each aligned block of 256 rows (0 to 255, 256 to 511, ...) at most 96 rows name the same one
- route_weight: float32 [2048, 2], P('ep'), may hold values from 0.1 to 1
- gate_weight: bfloat16 [8, 2048, 3584], P('ep', None, 'tp'), may hold values from -0.125 to 0.125
- up_weight: bfloat16 [8, 2048, 3584], P('ep', None, 'tp'), may hold values from -0.125 to 0.125
- down_weight: bfloat16 [8, 3584, 2048], P('ep', 'tp'), may hold values from -0.09375 to 0.09375
Outputs:
- mixer_out: bfloat16 [1024, 8192], P('tp', 'ep')
- expert_out: bfloat16 [2048, 2048], P('ep', 'tp')
The draws below stay inside these ranges and needn't reach their ends.
Inputs may be any that keep to these rules, and one draw needn't show every extreme that they name: `routes`: A row's 2 experts differ. Within the 256 rows of one index of ep, every expert is named at most 96 times; in some of these aligned blocks one expert is named exactly 96 times.
All inputs are finite; a program needn't handle non-finite values.
Results may differ from the reference program's by a relative error of at most 0.015.
Values may be sent and summed in bfloat16 or wider, within the bound.
A program may use at most 128 MiB of HBM per device.

```python
import math
import jax
import jax.numpy as jnp
import numpy as np
from jax import lax

D = 2048
HEADS = 16
HEAD_DIM = 64
WIDTH = 1024
FFX = 3584
TOPK = 2
BLOCK_TOKENS = 64
TOK_EP = 256
SEQ_DEV = 1024
EXPERTS = 8
CAP = 96
TOKENS = 2048
SEQUENCE_LENGTH = 8192
N_EP = 8
N_TP = 4


spike_count = 3


spike_total = 2


aligned_scale = 2.0


def head_classes(key):
    head_count = WIDTH // HEAD_DIM
    fast_count = head_count // 2
    order = jax.random.permutation(jax.random.fold_in(key, 101), head_count)
    return jnp.repeat(order < fast_count, HEAD_DIM)


def strong_cells(key):
    quick_decay_channels = head_classes(key)
    total_blocks = SEQUENCE_LENGTH // BLOCK_TOKENS
    selected_experts = jax.random.randint(jax.random.fold_in(key, 202), (spike_total,), 0, total_blocks)
    spike_token_rows = jnp.any((jnp.arange(SEQUENCE_LENGTH) // BLOCK_TOKENS)[:, None] == selected_experts[None, :], axis=1)
    return jnp.logical_or(quick_decay_channels[None, :], spike_token_rows[:, None])


def draw_key_in(key, part):
    random_keys = jax.random.split(jax.random.fold_in(key, 303), 3)
    strong = strong_cells(key)
    own_part = jnp.clip(jax.random.normal(random_keys[0], (SEQUENCE_LENGTH, WIDTH), jnp.float32), -4.0, 4.0)
    direction = jnp.clip(jax.random.normal(random_keys[1], (WIDTH,), jnp.float32), -3.0, 3.0)
    signs = (jax.random.randint(random_keys[2], (SEQUENCE_LENGTH,), 0, 2) * 2 - 1).astype(jnp.float32)
    shared = aligned_scale * signs[:, None] * direction[None, :]
    keys_drawn = jnp.where(strong, own_part + shared, own_part)
    return jnp.clip(keys_drawn, -10.0, 10.0).T.astype(jnp.bfloat16)


def draw_erase_pre(key, part):
    random_keys = jax.random.split(jax.random.fold_in(key, 404), 2)
    strong = strong_cells(key)
    high_value = jnp.clip(2.5 + 1.2 * jax.random.normal(random_keys[0], (SEQUENCE_LENGTH, WIDTH), jnp.float32), 0.5, 5.0)
    low_value = jnp.clip(-7.0 + 0.5 * jax.random.normal(random_keys[1], (SEQUENCE_LENGTH, WIDTH), jnp.float32), -8.0, -6.0)
    return jnp.where(strong, high_value, low_value).T.astype(jnp.bfloat16)


def draw_decay_pre(key, part):
    random_keys = jax.random.split(key, 7)
    slow_mask = jnp.logical_not(head_classes(key))
    slow_rate = jnp.log(1.0 / SEQUENCE_LENGTH) + jax.random.uniform(random_keys[1], (WIDTH,), jnp.float32, -1.0, 1.0)
    fast_rate = jax.random.uniform(random_keys[2], (WIDTH,), jnp.float32, jnp.log(1.0 / 100.0), jnp.log(1.0 / 30.0))
    base_rate = jnp.where(slow_mask, slow_rate, fast_rate)
    device_shift = jnp.repeat(jax.random.uniform(random_keys[3], (SEQUENCE_LENGTH // SEQ_DEV, 1), jnp.float32, -0.7, 0.7), SEQ_DEV, axis=0)
    jitter = jnp.clip(jax.random.normal(random_keys[4], (SEQUENCE_LENGTH, WIDTH), jnp.float32), -3.0, 3.0) * 0.6
    logarithm_rate = jnp.minimum(base_rate[None, :] + device_shift + jitter, -1.0)
    locations = jax.random.randint(random_keys[5], (spike_count,), 0, SEQUENCE_LENGTH)
    spike_rows = jnp.any(jnp.arange(SEQUENCE_LENGTH)[:, None] == locations[None, :], axis=1)
    dropped_share = jax.random.uniform(random_keys[6], (SEQUENCE_LENGTH, WIDTH), jnp.float32, 0.2, 0.45)
    spike_rate = jnp.log(-jnp.log(1.0 - dropped_share))
    logarithm_rate = jnp.where(spike_rows[:, None], spike_rate, logarithm_rate)
    return (-jnp.log(jnp.expm1(-logarithm_rate - 0.5))).T.astype(jnp.bfloat16)


def block_levels(key, extent, shards, low, top_value):
    level = 1.0
    for axis_at, parts in shards:
        heights = jax.random.uniform(jax.random.fold_in(jax.random.fold_in(key, 6), axis_at), (parts,), jnp.float32, low / len(shards), top_value / len(shards))
        level = level * jnp.repeat(jnp.exp(heights), extent[axis_at] // parts).reshape((-1,) + (1,) * (len(extent) - 1 - axis_at))
    return level


def shared_out(rng, own, number, rows, amount, top, most, lean):
    order = jax.random.permutation(rng, amount)
    crowded, usual = load_shares(amount, rows * top, most, lean, True), load_shares(amount, rows * top, most, lean, False)
    places = jnp.arange(amount)

    def named(sizes, rotation):
        used = int((sizes > 0).sum())
        fixed = max(1, used // 4)
        passed = fixed + (places - fixed + rotation * (used - fixed)) % max(1, amount - fixed)
        return jnp.zeros((amount,), jnp.int32).at[order[jnp.where(places < fixed, places, passed)]].set(jnp.asarray(sizes, jnp.int32))

    sizes = jnp.where(number % 4 == 0, named(crowded, number // 4), named(usual, number - number // 4 - 1))
    mixed = jax.random.permutation(jax.random.fold_in(own, 3), amount)
    giver, receiver = mixed[0:amount // 2 * 2:2], mixed[1:amount // 2 * 2:2]
    slack = jnp.minimum(sizes[giver] - 1, most - sizes[receiver]) // 2
    slack = jnp.where((giver == order[0]) | (receiver == order[0]) | (sizes[receiver] == 0), 0, jnp.maximum(slack, 0))
    passed = jax.random.randint(jax.random.fold_in(own, 4), (amount // 2,), 0, 1 << 20) % (slack + 1)
    sizes = sizes.at[giver].add(-passed).at[receiver].add(passed)
    members = jnp.searchsorted(jnp.cumsum(sizes), jnp.arange(rows * top), side="right").astype(jnp.int32)
    listing = members.reshape(top, rows).T
    listing = listing[jax.random.permutation(jax.random.fold_in(own, 1), rows)]
    rotation = jax.random.randint(jax.random.fold_in(own, 2), (rows, 1), 0, top)
    return jnp.take_along_axis(listing, (jnp.arange(top)[None, :] + rotation) % top, axis=1)


def load_shares(number_of, total, limit, slope, full):
    portions = [(1 << 20) // math.isqrt(rank ** slope) + 1 for rank in range(1, number_of + 1)]
    largest = limit if full else min(limit, max(-(-total // number_of), total * portions[0] // sum(portions)))
    least = 1 if total - largest >= number_of - 1 else 0
    given, spare = [largest] + [least] * (number_of - 1), total - largest - least * (number_of - 1)
    while spare > 0:
        free = [i for i in range(1, number_of) if given[i] < largest] or [i for i in range(1, number_of) if given[i] < limit]
        mass, budget = sum([portions[i] for i in free]), spare
        for i in free:
            more = min(limit - given[i], max(1, budget * portions[i] // mass), spare)
            given[i] = given[i] + more
            spare = spare - more
    return np.array(given)


def gaussian(stream_key, dims, width, bound, cuts=(), kind=jnp.bfloat16):
    values = width * jax.random.normal(stream_key, dims, jnp.float32)
    if cuts:
        values = values * block_levels(stream_key, dims, cuts, -0.22, 0.18)
    return jnp.clip(values, -bound, bound).astype(kind)


def setup_inputs(seed: int = 0) -> dict:
    streams_of = jax.random.split(jax.random.key(seed), 14)
    query_in = gaussian(streams_of[0], (WIDTH, SEQUENCE_LENGTH), 1.0, 6.0, ((0, 4), (1, 8)))
    key_in = draw_key_in(jax.random.fold_in(streams_of[13], 71), 0)
    value_in = gaussian(streams_of[2], (WIDTH, SEQUENCE_LENGTH), 1.0, 6.0, ((0, 4), (1, 8)))
    erase_pre = draw_erase_pre(jax.random.fold_in(streams_of[13], 71), 0)
    decay_pre = draw_decay_pre(jax.random.fold_in(streams_of[13], 71), 0)
    mix_gain = jnp.clip(1.0 + 0.18 * jax.random.normal(streams_of[5], (WIDTH,), jnp.float32), 0.1, 1.9)
    expert_in = gaussian(streams_of[6], (TOKENS, D), 1.0, 6.0, ((0, 8),))
    expert_gain = jnp.clip(1.0 + 0.18 * jax.random.normal(streams_of[7], (D,), jnp.float32), 0.1, 1.9)
    routes_keys = jax.random.split(jax.random.fold_in(streams_of[8], 1), TOKENS // TOK_EP)
    routes_turns = jax.random.permutation(jax.random.fold_in(streams_of[8], 3), TOKENS // TOK_EP)
    routes = jax.vmap(lambda own, number: shared_out(jax.random.fold_in(streams_of[8], 2), own, number, TOK_EP, EXPERTS, TOPK, CAP, 2))(routes_keys, routes_turns).reshape((TOKENS, TOPK))
    route_weight = jnp.clip(0.1 + 0.9 * jax.random.uniform(streams_of[9], (TOKENS, TOPK), jnp.float32) ** block_levels(streams_of[9], (TOKENS, TOPK), ((0, 8),), -0.2, 0.2), 0.1, 1.0)
    gate_weight = gaussian(streams_of[10], (EXPERTS, D, FFX), D ** -0.5, 0.125, ((0, 8), (2, 4)))
    up_weight = gaussian(streams_of[11], (EXPERTS, D, FFX), D ** -0.5, 0.125, ((0, 8), (2, 4)))
    down_weight = gaussian(streams_of[12], (EXPERTS, FFX, D), FFX ** -0.5, 0.09375, ((0, 8), (1, 4)))
    return {"query_in": query_in, "key_in": key_in, "value_in": value_in, "erase_pre": erase_pre, "decay_pre": decay_pre, "mix_gain": mix_gain, "expert_in": expert_in, "expert_gain": expert_gain, "routes": routes, "route_weight": route_weight, "gate_weight": gate_weight, "up_weight": up_weight, "down_weight": down_weight}


highest = lax.Precision.HIGHEST

def token_terms(key_in, erase_pre, decay_pre):
    key_f = key_in.astype(jnp.float32)
    unit_key = key_f * lax.rsqrt(lax.optimization_barrier(jnp.sum(key_f * key_f, axis=-1, keepdims=True)) + 1e-05)
    eraser = unit_key * jax.nn.sigmoid(erase_pre.astype(jnp.float32))
    log_keep = -jnp.exp(-jax.nn.softplus(-decay_pre.astype(jnp.float32)) - 0.5)
    return (key_f, unit_key, eraser, log_keep)

def advance(carried, inputs):
    query_f, key_f, value_f, unit_key, eraser, keep = inputs
    seen = jnp.einsum('hvk,hk->hv', carried, unit_key, precision=highest)
    carried = carried * keep[:, None, :] - seen[:, :, None] * eraser[:, None, :] + value_f[:, :, None] * key_f[:, None, :]
    return (carried, jnp.einsum('hvk,hk->hv', carried, query_f, precision=highest))

def mixer(query_in, key_in, value_in, erase_pre, decay_pre, mix_gain):
    layout = (SEQUENCE_LENGTH, HEADS, HEAD_DIM)
    query_f = query_in.astype(jnp.float32).reshape(layout)
    value_f = value_in.astype(jnp.float32).reshape(layout)
    key_f, unit_key, eraser, log_keep = token_terms(key_in.reshape(layout), erase_pre.reshape(layout), decay_pre.reshape(layout))
    inputs = (query_f, key_f, value_f, unit_key, eraser, jnp.exp(log_keep))
    initial = jnp.zeros((HEADS, HEAD_DIM, HEAD_DIM), jnp.float32)
    _, ahead = lax.scan(advance, initial, inputs)
    _, behind = lax.scan(advance, initial, inputs, reverse=True)
    summed = ahead + behind
    center = lax.optimization_barrier(jnp.mean(summed, axis=-1, keepdims=True))
    spread = lax.optimization_barrier(jnp.mean(jnp.square(summed - center), axis=-1, keepdims=True))
    scaled = (summed - center) * lax.rsqrt(spread + HEAD_DIM * 1e-05) * mix_gain.reshape(HEADS, HEAD_DIM)
    return scaled.astype(jnp.bfloat16).reshape(SEQUENCE_LENGTH, HEADS * HEAD_DIM)

def slot_targets(routes):
    onehot = (routes[:, :, None] == jnp.arange(EXPERTS, dtype=jnp.int32)[None, None, :]).astype(jnp.int32)
    flat = onehot.reshape(-1, EXPERTS)
    before = jnp.cumsum(flat, axis=0) - flat
    slot_index = lax.optimization_barrier(jnp.sum(before * flat, axis=-1)).reshape(routes.shape)
    return routes * CAP + slot_index

def dispatch_matrix(targets, slot_total):
    matches = targets[None, :, :] == jnp.arange(slot_total, dtype=jnp.int32)[:, None, None]
    return lax.optimization_barrier(jnp.sum(matches.astype(jnp.float32), axis=-1)).astype(jnp.bfloat16)

def experts_part(expert_in, expert_gain, routes, route_weight, gate_weight, up_weight, down_weight):
    input_f = expert_in.astype(jnp.float32)
    normed = (input_f * lax.rsqrt(lax.optimization_barrier(jnp.mean(input_f * input_f, axis=-1, keepdims=True)) + 1e-06) * expert_gain).astype(jnp.bfloat16)
    targets = jax.vmap(slot_targets)(routes.reshape(N_EP, TOK_EP, TOPK))

    def fill(pack):
        selected_experts, rows = pack
        return jnp.dot(dispatch_matrix(selected_experts, EXPERTS * CAP), rows, preferred_element_type=jnp.float32).astype(jnp.bfloat16)
    buffers = lax.map(fill, (targets, normed.reshape(N_EP, TOK_EP, D)))
    buffers = buffers.reshape(N_EP, EXPERTS, CAP, D).transpose(1, 0, 2, 3).reshape(EXPERTS, N_EP * CAP, D)

    def expert(pack):
        rows, gate_mat, up_mat, down_mat = pack
        gate_sum = jnp.dot(rows, gate_mat, preferred_element_type=jnp.float32)
        up_sum = jnp.dot(rows, up_mat, preferred_element_type=jnp.float32)
        hidden = (jax.nn.silu(gate_sum) * up_sum).astype(jnp.bfloat16)
        groups = hidden.reshape(-1, N_TP, FFX // N_TP).astype(jnp.float32)
        downs = down_mat.reshape(N_TP, FFX // N_TP, D).astype(jnp.float32)
        partial_value = jnp.einsum('rjf,jfd->jrd', groups, downs).astype(jnp.bfloat16)
        partial_value = lax.optimization_barrier(partial_value)
        return lax.optimization_barrier(jnp.sum(partial_value.astype(jnp.float32), axis=0)).astype(jnp.bfloat16)
    results = lax.map(expert, (buffers, gate_weight, up_weight, down_weight)).reshape(EXPERTS, N_EP, CAP, D)
    source = (jnp.arange(TOKENS, dtype=jnp.int32) // TOK_EP)[:, None]
    slot_index = targets.reshape(TOKENS, TOPK) - routes * CAP
    picked = results[routes, source, slot_index].astype(jnp.float32)
    return lax.optimization_barrier(jnp.sum(picked * route_weight[:, :, None], axis=1)).astype(jnp.bfloat16)

def reference(query_in, key_in, value_in, erase_pre, decay_pre, mix_gain, expert_in, expert_gain, routes, route_weight, gate_weight, up_weight, down_weight):
    mixer_out = mixer(query_in.T, key_in.T, value_in.T, erase_pre.T, decay_pre.T, mix_gain).T
    expert_out = experts_part(expert_in, expert_gain, routes, route_weight, gate_weight, up_weight, down_weight)
    return (mixer_out, expert_out)
```

```python
import functools
import math

import jax
import jax.numpy as jnp
from jax import lax
from jax.experimental import pallas as pl
from jax.experimental.pallas import tpu as pltpu
from jax.sharding import PartitionSpec as P

HEAD_DIM = 64


highest = lax.Precision.HIGHEST
SPAN = 128
GROUPS = 4
MESH = pl.DeviceIdType.MESH


def dot(left, right, dims=((1,), (0,)), precision=None):
    return lax.dot_general(
        left, right, (dims, ((), ())), precision=precision, preferred_element_type=jnp.float32
    )


def low(array):
    return array.astype(jnp.bfloat16)


TN = ((0,), (0,))
NT = ((1,), (1,))


def flipped(index, bits):
    bit = 1
    out = index
    while bit <= bits:
        if bits & bit:
            out = out + bit - 2 * bit * lax.rem(lax.div(index, bit), 2)
        bit *= 2
    return out


def greet(ep_count, tp_count, mine, column):
    barrier = pltpu.get_barrier_semaphore()
    for s in range(1, ep_count):
        pl.semaphore_signal(
            barrier, inc=1, device_id={"ep": flipped(mine, s)}, device_id_type=MESH
        )
    for p in range(1, tp_count):
        pl.semaphore_signal(
            barrier, inc=1, device_id={"tp": flipped(column, p)}, device_id_type=MESH
        )
    pl.semaphore_wait(barrier, ep_count + tp_count - 2)


def local_block(c, q_ref, k_ref, v_ref, e_ref, d_ref, read_ref, out_ref, step_ref, map_ref):
    channels = q_ref.shape[0]
    span = SPAN
    heads = channels // HEAD_DIM
    tokens = pl.ds(pl.multiple_of(c * span, span), span)
    row = lax.broadcasted_iota(jnp.int32, (span, span), 0)
    col = lax.broadcasted_iota(jnp.int32, (span, span), 1)
    crossed = row ^ col

    query_f = q_ref[:, tokens].astype(jnp.float32)
    key_f = k_ref[:, tokens].astype(jnp.float32)
    value = v_ref[:, tokens]
    log_keep = -math.exp(-0.5) / (1.0 + jnp.exp(-d_ref[:, tokens].astype(jnp.float32)))
    squares = (key_f * key_f).reshape(heads, HEAD_DIM, span)
    norm = lax.rsqrt(jnp.sum(squares, axis=1, keepdims=True) + 1e-05)
    unit = (key_f.reshape(heads, HEAD_DIM, span) * norm).reshape(channels, span)
    eraser = unit / (1.0 + jnp.exp(-e_ref[:, tokens].astype(jnp.float32)))

    upper = jnp.where(row <= col, 1.0, 0.0)
    cumulative = dot(log_keep, upper, precision=highest)
    prior = cumulative - log_keep
    total = cumulative[:, span - 1 :]
    middle = cumulative[:, span // 2 - 1 : span // 2]
    prior_up = jnp.exp(prior - middle)
    cum_down = jnp.exp(middle - cumulative)
    cum_up = jnp.exp(cumulative - middle)
    prior_down = jnp.exp(middle - prior)
    to_middle = jnp.exp(middle)
    from_middle = jnp.exp(total - middle)
    decay = jnp.exp(total)

    sides = (
        (unit * prior_up, query_f * cum_up, key_f * cum_down, eraser * cum_down,
         to_middle, from_middle, row < col, row <= col),
        (unit * cum_down, query_f * prior_down, key_f * prior_up, eraser * prior_up,
         from_middle, to_middle, row > col, row >= col),
    )
    units = []
    for side, (u, q, k, e, scale_in, scale_out, strict, inclusive) in enumerate(sides):
        u0, q0 = u * scale_in, q * scale_in
        for h in range(heads):
            at = slice(h * HEAD_DIM, (h + 1) * HEAD_DIM)
            uq = jnp.concatenate([low(u[at]), low(q[at])], axis=1)
            kb, eb = low(k[at]), low(e[at])
            mk = dot(kb, uq, TN)
            me = dot(eb, uq, TN)
            erase_mix = jnp.where(strict, me[:, :span], 0.0)
            units.append(
                dict(
                    side=side, h=h, at=at, kb=kb, eb=eb, u0=u0[at], q0=q0[at],
                    key_mix=low(jnp.where(strict, mk[:, :span], 0.0)),
                    key_read=low(jnp.where(inclusive, mk[:, span:], 0.0)),
                    erase_read=low(jnp.where(inclusive, me[:, span:], 0.0)),
                    erase_mix=erase_mix,
                    scale_out=scale_out[at], decay=decay[at],
                )
            )
    eye = jnp.where(row == col, 1.0, 0.0)
    solved = [eye - jnp.where(crossed == 1, m["erase_mix"], 0.0) for m in units]
    level = 1
    while (1 << level) < span:
        mask = (crossed >> level) == 1
        held = [low(x) for x in solved]
        half = [
            low(dot(x, low(jnp.where(mask, m["erase_mix"], 0.0)))) for x, m in zip(held, units)
        ]
        solved = [s - dot(y, x) for s, y, x in zip(solved, half, held)]
        level += 1

    outs = [None] * heads
    eye_k = jnp.where(
        lax.broadcasted_iota(jnp.int32, (HEAD_DIM, HEAD_DIM), 0)
        == lax.broadcasted_iota(jnp.int32, (HEAD_DIM, HEAD_DIM), 1),
        1.0,
        0.0,
    )
    for m, x in zip(units, solved):
        v = value[m["at"]]
        vm = dot(v, jnp.concatenate([m["key_mix"], m["key_read"]], axis=1))
        stacked = jnp.concatenate([low(vm[:, :span]), low(m["u0"])], axis=0)
        removed = low(dot(stacked, low(x)))
        taken = dot(removed, m["erase_read"])
        local = vm[:, span:] - taken[:HEAD_DIM]
        h, side = m["h"], m["side"]
        outs[h] = local if outs[h] is None else outs[h] + local
        read_ref[side, m["at"], tokens] = low(m["q0"] - taken[HEAD_DIM:])
        gone = dot(m["eb"], removed, NT)
        added = dot(m["kb"], v, NT)
        state = (added - gone[:, :HEAD_DIM]) * m["scale_out"]
        moved = eye_k * m["decay"] - gone[:, HEAD_DIM:] * m["scale_out"]
        step_ref[c, side, h] = jnp.concatenate([state, moved], axis=1)
    for h in range(heads):
        out_ref[h * HEAD_DIM : (h + 1) * HEAD_DIM, tokens] = outs[h]

    none = jnp.zeros_like(eye_k)
    for h in range(heads):
        step = step_ref[c, 0, h]
        new = dot(step[:, HEAD_DIM:], map_ref[0, h], precision=highest)
        map_ref[0, h] = new + jnp.concatenate([step[:, :HEAD_DIM], none], axis=1)
        before = map_ref[1, h]
        new = dot(before[:, HEAD_DIM:], step_ref[c, 1, h], precision=highest)
        map_ref[1, h] = new + jnp.concatenate([before[:, :HEAD_DIM], none], axis=1)


def outbound_kernel(
    ep_count, tp_count, buffer_ref, q_ref, k_ref, v_ref, e_ref, d_ref,
    arrived_ref, read_ref, out_ref, step_ref, sent_map_ref,
    map_ref, own_sem, send_z, recv_z, send_t, recv_t,
):
    mine, column = lax.axis_index("ep"), lax.axis_index("tp")
    blocks = q_ref.shape[1] // SPAN
    width = buffer_ref.shape[2]
    groups = min(GROUPS, ep_count)
    per = ep_count // groups
    part = pl.ds(pl.multiple_of(column * width, width), width)
    greet(ep_count, tp_count, mine, column)

    away = {}
    for s in range(1, ep_count):
        target = flipped(mine, s)
        away[s] = pltpu.make_async_remote_copy(
            src_ref=buffer_ref.at[target],
            dst_ref=arrived_ref.at[mine, :, part],
            send_sem=send_z.at[s],
            recv_sem=recv_z.at[s],
            device_id={"ep": target},
            device_id_type=MESH,
        )
        away[s].start()
    own = pltpu.make_async_copy(buffer_ref.at[mine], arrived_ref.at[mine, :, part], own_sem)
    own.start()
    own.wait()

    spread = []
    for k in range(groups):
        first = flipped(lax.div(mine, per), k) * per
        block = arrived_ref.at[pl.ds(first, per), :, part]
        spread.append(
            [
                pltpu.make_async_remote_copy(
                    src_ref=block,
                    dst_ref=block,
                    send_sem=send_t.at[k, p],
                    recv_sem=recv_t.at[k, p],
                    device_id={"tp": flipped(column, p)},
                    device_id_type=MESH,
                )
                for p in range(1, tp_count)
            ]
        )

    def pass_on(k):
        for s in range(max(1, k * per), (k + 1) * per):
            away[s].wait_recv()
        for copy in spread[k]:
            copy.start()

    pass_on(0)
    for h in range(map_ref.shape[1]):
        start = jnp.concatenate(
            [
                jnp.zeros((HEAD_DIM, HEAD_DIM), jnp.float32),
                jnp.where(
                    lax.broadcasted_iota(jnp.int32, (HEAD_DIM, HEAD_DIM), 0)
                    == lax.broadcasted_iota(jnp.int32, (HEAD_DIM, HEAD_DIM), 1),
                    1.0,
                    0.0,
                ),
            ],
            axis=1,
        )
        map_ref[0, h] = start
        map_ref[1, h] = start

    when = [min(e, blocks - 1) for e in (0, 1, 2, 4)]

    def work(c, carry):
        for k in range(1, groups):

            @pl.when(c == when[k])
            def _():
                pass_on(k)

        local_block(c, q_ref, k_ref, v_ref, e_ref, d_ref, read_ref, out_ref, step_ref, map_ref)
        return carry

    lax.fori_loop(0, blocks, work, 0)
    sent_map_ref[...] = low(map_ref[...])
    for k in range(groups):
        for copy in spread[k]:
            copy.wait_recv()
            copy.wait_send()
    for s in range(1, ep_count):
        away[s].wait_send()


def inbound_kernel(
    ep_count, tp_count, part_ref, maps_ref, step_ref, read_ref, local_ref, gain_ref,
    out_ref, returned_ref,
    total_ref, peers_ref, gathered_ref, enter_ref, states_ref,
    send_m, recv_m, send_t, recv_t, send_z, recv_z,
):
    mine, column = lax.axis_index("ep"), lax.axis_index("tp")
    heads = maps_ref.shape[1]
    blocks = step_ref.shape[0]
    width = returned_ref.shape[2]
    groups = min(GROUPS, ep_count)
    per = ep_count // groups
    greet(ep_count, tp_count, mine, column)

    order = list(range(groups))[::-1]
    shares = {}
    for k in order:
        rows = pl.ds(flipped(lax.div(mine, per), k) * per, per)
        for p in range(1, tp_count):
            target = flipped(column, p)
            shares[k, p] = pltpu.make_async_remote_copy(
                src_ref=part_ref.at[rows, :, pl.ds(pl.multiple_of(target * width, width), width)],
                dst_ref=peers_ref.at[p - 1, rows],
                send_sem=send_t.at[k, p],
                recv_sem=recv_t.at[k, p],
                device_id={"tp": target},
                device_id_type=MESH,
            )
            shares[k, p].start()
    sides = {}
    for s in range(1, ep_count):
        target = lax.rem(mine + s, ep_count)
        sides[s] = pltpu.make_async_remote_copy(
            src_ref=maps_ref.at[lax.div(mine + s, ep_count)],
            dst_ref=gathered_ref.at[mine],
            send_sem=send_m.at[s],
            recv_sem=recv_m.at[s],
            device_id={"ep": target},
            device_id_type=MESH,
        )
        sides[s].start()

    back = {}
    for s in range(1, ep_count):
        target = flipped(mine, s)
        back[s] = pltpu.make_async_remote_copy(
            src_ref=total_ref.at[target],
            dst_ref=returned_ref.at[mine],
            send_sem=send_z.at[s],
            recv_sem=recv_z.at[s],
            device_id={"ep": target},
            device_id_type=MESH,
        )

    def give_back(k):
        first = flipped(lax.div(mine, per), k) * per
        for p in range(1, tp_count):
            shares[k, p].wait_recv()
        for r in range(per):
            own = pl.ds(pl.multiple_of(column * width, width), width)
            total = part_ref[first + r, :, own].astype(jnp.float32)
            for p in range(1, tp_count):
                total = total + peers_ref[p - 1, first + r].astype(jnp.float32)
            total_ref[first + r] = low(total)
        for s in range(k * per, (k + 1) * per):
            if s:
                back[s].start()
            else:
                returned_ref[mine] = total_ref[mine]

    enter_ref[...] = jnp.zeros_like(enter_ref)
    for s in range(1, ep_count):
        sides[s].wait_recv()

    def gather(j, carry):
        for side, at in ((0, j), (1, ep_count - 1 - j)):
            reached = at < mine if side == 0 else at > mine

            @pl.when(reached)
            def _():
                for h in range(heads):
                    part = gathered_ref[at, h]
                    state = enter_ref[side, h]
                    high = low(state)
                    rest = low(state - high.astype(jnp.float32))
                    both = jnp.concatenate([high, rest], axis=1)
                    new = dot(part[:, HEAD_DIM:], both)
                    enter_ref[side, h] = (
                        new[:, :HEAD_DIM] + new[:, HEAD_DIM:] + part[:, :HEAD_DIM].astype(jnp.float32)
                    )

        return carry

    lax.fori_loop(0, ep_count, gather, 0)

    def chain(j, carry):
        for side, at in ((0, j), (1, blocks - 1 - j)):
            for h in range(heads):
                step = step_ref[at, side, h]
                state = enter_ref[side, h]
                states_ref[at, h, side * HEAD_DIM : (side + 1) * HEAD_DIM, :] = low(state)
                enter_ref[side, h] = step[:, :HEAD_DIM] + dot(
                    step[:, HEAD_DIM:], state, precision=highest
                )
        return carry

    lax.fori_loop(0, blocks, chain, 0)

    when = {order[0]: 0}
    if groups > 1:
        when[order[1]] = blocks // 2

    def write(j, carry):
        for k, at in when.items():

            @pl.when(j == at)
            def _():
                give_back(k)

        tokens = pl.ds(pl.multiple_of(j * SPAN, SPAN), SPAN)
        for h in range(heads):
            at = slice(h * HEAD_DIM, (h + 1) * HEAD_DIM)
            reads = jnp.concatenate([read_ref[0, at, tokens], read_ref[1, at, tokens]], axis=0)
            summed = local_ref[at, tokens] + dot(states_ref[j, h], reads, TN)
            center = jnp.mean(summed, axis=0, keepdims=True)
            moved = summed - center
            spread = jnp.mean(moved * moved, axis=0, keepdims=True)
            scaled = moved * lax.rsqrt(spread + HEAD_DIM * 1e-05) * gain_ref[at, :]
            out_ref[at, tokens] = low(scaled)
        return carry

    lax.fori_loop(0, blocks, write, 0)
    for k in order:
        if k not in when:
            give_back(k)
    for s in range(1, ep_count):
        back[s].wait_recv()
        back[s].wait_send()
        sides[s].wait_send()
    for copy in shares.values():
        copy.wait_send()


def outbound(buffer, query_in, key_in, value_in, erase_pre, decay_pre):
    channels, seq_len = query_in.shape
    ep_count, capacity, width = buffer.shape
    tp_count = lax.axis_size("tp")
    heads = channels // HEAD_DIM
    blocks = seq_len // SPAN
    groups = min(GROUPS, ep_count)
    f32 = jnp.float32
    whole = pl.BlockSpec(memory_space=pltpu.VMEM)
    dma = pltpu.SemaphoreType.DMA
    return pl.pallas_call(
        functools.partial(outbound_kernel, ep_count, tp_count),
        in_specs=[whole] * 6,
        out_specs=[whole] * 5,
        out_shape=[
            jax.ShapeDtypeStruct((ep_count, capacity, width * tp_count), jnp.bfloat16),
            jax.ShapeDtypeStruct((2, channels, seq_len), jnp.bfloat16),
            jax.ShapeDtypeStruct((channels, seq_len), f32),
            jax.ShapeDtypeStruct((blocks, 2, heads, HEAD_DIM, 2 * HEAD_DIM), f32),
            jax.ShapeDtypeStruct((2, heads, HEAD_DIM, 2 * HEAD_DIM), jnp.bfloat16),
        ],
        scratch_shapes=[
            pltpu.VMEM((2, heads, HEAD_DIM, 2 * HEAD_DIM), f32),
            dma,
            dma((ep_count,)),
            dma((ep_count,)),
            dma((groups, tp_count)),
            dma((groups, tp_count)),
        ],
        compiler_params=pltpu.CompilerParams(collective_id=0, has_side_effects=True),
        cost_estimate=pl.CostEstimate(
            flops=int(4e10 * heads * blocks / 32), bytes_accessed=1 << 23, transcendentals=1 << 20
        ),
        name="outbound",
    )(buffer, query_in, key_in, value_in, erase_pre, decay_pre)


def inbound(part, maps, steps, reads, local, mix_gain):
    channels, seq_len = local.shape
    ep_count, capacity, features = part.shape
    tp_count = lax.axis_size("tp")
    width = features // tp_count
    blocks, _, heads = steps.shape[:3]
    groups = min(GROUPS, ep_count)
    f32 = jnp.float32
    whole = pl.BlockSpec(memory_space=pltpu.VMEM)
    dma = pltpu.SemaphoreType.DMA
    return pl.pallas_call(
        functools.partial(inbound_kernel, ep_count, tp_count),
        in_specs=[whole] * 6,
        out_specs=[whole] * 2,
        out_shape=[
            jax.ShapeDtypeStruct((channels, seq_len), jnp.bfloat16),
            jax.ShapeDtypeStruct((ep_count, capacity, width), jnp.bfloat16),
        ],
        scratch_shapes=[
            pltpu.VMEM((ep_count, capacity, width), jnp.bfloat16),
            pltpu.VMEM((tp_count - 1, ep_count, capacity, width), jnp.bfloat16),
            pltpu.VMEM((ep_count, heads, HEAD_DIM, 2 * HEAD_DIM), jnp.bfloat16),
            pltpu.VMEM((2, heads, HEAD_DIM, HEAD_DIM), f32),
            pltpu.VMEM((blocks, heads, 2 * HEAD_DIM, HEAD_DIM), jnp.bfloat16),
            dma((ep_count,)),
            dma((ep_count,)),
            dma((groups, tp_count)),
            dma((groups, tp_count)),
            dma((ep_count,)),
            dma((ep_count,)),
        ],
        compiler_params=pltpu.CompilerParams(collective_id=1, has_side_effects=True),
        cost_estimate=pl.CostEstimate(
            flops=int(1e10 * heads * blocks / 32), bytes_accessed=1 << 23, transcendentals=1 << 14
        ),
        name="inbound",
    )(part, maps, steps, reads, local, mix_gain.reshape(channels, 1))


def slot_targets(routes, experts_n, capacity):
    onehot = (routes[:, :, None] == jnp.arange(experts_n, dtype=jnp.int32)[None, None, :]).astype(
        jnp.int32
    )
    flat = onehot.reshape(-1, experts_n)
    before = jnp.cumsum(flat, axis=0) - flat
    slot_index = jnp.sum(before * flat, axis=-1).reshape(routes.shape)
    return routes * capacity + slot_index


def dispatch_matrix(targets, slot_total):
    matches = targets[None, :, :] == jnp.arange(slot_total, dtype=jnp.int32)[:, None, None]
    return jnp.sum(matches.astype(jnp.float32), axis=-1).astype(jnp.bfloat16)


def on_device(
    query_in,
    key_in,
    value_in,
    erase_pre,
    decay_pre,
    mix_gain,
    expert_in,
    expert_gain,
    routes,
    route_weight,
    gate_weight,
    up_weight,
    down_weight,
):
    experts_n = lax.axis_size("ep")
    row_count = expert_in.shape[0]
    capacity = 3 * routes.shape[1] * row_count // (2 * experts_n)
    slot_total = experts_n * capacity
    input_f = expert_in.astype(jnp.float32)
    normed = (
        input_f
        * lax.rsqrt(jnp.mean(input_f * input_f, axis=-1, keepdims=True) + 1e-06)
        * expert_gain
    ).astype(jnp.bfloat16)
    targets = slot_targets(routes, experts_n, capacity)
    col_count = normed.shape[1] // lax.axis_size("tp")
    mine = lax.dynamic_slice_in_dim(normed, lax.axis_index("tp") * col_count, col_count, 1)
    buffer = jnp.dot(
        dispatch_matrix(targets, slot_total), mine, preferred_element_type=jnp.float32
    ).astype(jnp.bfloat16)
    arrived, reads, local, steps, maps = outbound(
        buffer.reshape(experts_n, capacity, col_count),
        query_in, key_in, value_in, erase_pre, decay_pre,
    )
    arrived = arrived.reshape(slot_total, -1)
    gate_sum = jnp.dot(arrived, gate_weight[0], preferred_element_type=jnp.float32)
    up_sum = jnp.dot(arrived, up_weight[0], preferred_element_type=jnp.float32)
    hidden = (jax.nn.silu(gate_sum) * up_sum).astype(jnp.bfloat16)
    part = jnp.dot(hidden, down_weight[0], preferred_element_type=jnp.float32).astype(jnp.bfloat16)
    mixer_out, returned = inbound(
        part.reshape(experts_n, capacity, -1), maps, steps, reads, local, mix_gain
    )
    returned = returned.reshape(slot_total, col_count)
    matches = targets[:, :, None] == jnp.arange(slot_total, dtype=jnp.int32)[None, None, :]
    combine = jnp.sum(matches.astype(jnp.float32) * route_weight[:, :, None], axis=1)
    result = jnp.dot(combine, returned.astype(jnp.float32), precision=highest)
    return (mixer_out, result.astype(jnp.bfloat16))


def solution(mesh):
    placed = (
        P("tp", "ep"),
        P("tp", "ep"),
        P("tp", "ep"),
        P("tp", "ep"),
        P("tp", "ep"),
        P("tp"),
        P("ep", None),
        P(),
        P("ep", None),
        P("ep", None),
        P("ep", None, "tp"),
        P("ep", None, "tp"),
        P("ep", "tp", None),
    )
    return jax.shard_map(
        on_device,
        mesh=mesh,
        in_specs=placed,
        out_specs=(P("tp", "ep"), P("ep", "tp")),
        check_vma=False,
    )
```

```python
import functools
import math

import jax
import jax.numpy as jnp
from jax import lax
from jax.experimental import pallas as pl
from jax.experimental.pallas import tpu as pltpu
from jax.sharding import PartitionSpec as P

HEAD_DIM = 64


highest = lax.Precision.HIGHEST
SPAN = 128
GROUPS = 4
PAIR = 2
ROWS = 32
PLAN = (
    "c0", "p0", "P1", "S0", "m0", "m1", "P2", "m2", "P3", "F2", "m3", "F3", "M0", "R0", "c2",
    "p2", "S2", "c3", "p3", "R2", "S3", "c1", "p1", "B2", "S1", "R3", "E0", "B3", "R1", "W0",
    "W1", "B1", "B0",
)
MESH = pl.DeviceIdType.MESH


def dot(left, right, dims=((1,), (0,)), precision=None):
    return lax.dot_general(
        left, right, (dims, ((), ())), precision=precision, preferred_element_type=jnp.float32
    )


def low(array):
    return array.astype(jnp.bfloat16)


TN = ((0,), (0,))
NT = ((1,), (1,))


def flipped(index, bits, limit=GROUPS):
    out = index
    bit = 1
    while bit < (2 * bits if isinstance(bits, int) else limit):
        if not isinstance(bits, int):
            theirs = lax.rem(lax.div(bits, bit), 2)
            out = out + bit * theirs * (1 - 2 * lax.rem(lax.div(index, bit), 2))
        elif bits & bit:
            out = out + bit - 2 * bit * lax.rem(lax.div(index, bit), 2)
        bit *= 2
    return out


def remote(axis, target, source, there, send, recv):
    return pltpu.make_async_remote_copy(
        src_ref=source,
        dst_ref=there,
        send_sem=send,
        recv_sem=recv,
        device_id={axis: target},
        device_id_type=MESH,
    )


def greet(ep_count, tp_count, mine, column):
    barrier = pltpu.get_barrier_semaphore()
    for s in range(1, ep_count):
        pl.semaphore_signal(
            barrier, inc=1, device_id={"ep": flipped(mine, s)}, device_id_type=MESH
        )
    for p in range(1, tp_count):
        pl.semaphore_signal(
            barrier, inc=1, device_id={"tp": flipped(column, p)}, device_id_type=MESH
        )
    return lambda: pl.semaphore_wait(barrier, ep_count + tp_count - 2)


def split(array):
    high = low(array)
    return high, low(array - high.astype(jnp.float32))


def close_dot(left, right):
    lh, ll = split(left)
    rh, rl = split(right)
    return dot(
        jnp.concatenate([lh, lh, ll], axis=1), jnp.concatenate([rh, rl, rh], axis=0)
    )


def level_count():
    return SPAN.bit_length() - 1


def write_masks(mask_ref, fold_ref):
    row = lax.broadcasted_iota(jnp.int32, (SPAN, SPAN), 0)
    col = lax.broadcasted_iota(jnp.int32, (SPAN, SPAN), 1)
    crossed = row ^ col

    def pick(test):
        return low(jnp.where(test, 1.0, 0.0))

    near = (crossed >> (level_count() - 1)) == 0
    mask_ref[0], mask_ref[1] = pick(row < col), pick(row > col)
    mask_ref[2], mask_ref[3] = pick(row <= col), pick(row >= col)
    mid = SPAN // 2
    half_row = lax.broadcasted_iota(jnp.int32, (mid, SPAN), 0)
    half_col = lax.broadcasted_iota(jnp.int32, (mid, SPAN), 1)
    over = half_col >= mid
    folded = half_col - jnp.where(over, mid, 0)
    for level in range(1, level_count()):
        mask_ref[2 + 2 * level] = pick((crossed >> level) == 1)
        odd = (row >> level) % 2
        inside = jnp.where(odd == 1, col - row, row - col) >= 0
        mask_ref[3 + 2 * level] = pick(jnp.logical_and(near, inside))
        odd = ((half_row + jnp.where(over, mid, 0)) >> level) % 2
        fold_ref[level - 1] = pick(jnp.where(odd == 1, half_row - folded, folded - half_row) >= 0)
    fold_ref[level_count() - 1] = pick(half_row <= folded)
    fold_ref[level_count()] = pick(half_row >= folded)


def local_block(
    pair, q_ref, k_ref, v_ref, e_ref, d_ref, read_ref, out_ref, step_ref, map_ref, mask_ref, fold_ref
):
    channels = q_ref.shape[0]
    span = SPAN
    mid = span // 2
    heads = channels // HEAD_DIM
    levels = level_count()
    row = lax.broadcasted_iota(jnp.int32, (span, span), 0)
    col = lax.broadcasted_iota(jnp.int32, (span, span), 1)
    half_row = lax.broadcasted_iota(jnp.int32, (mid, span), 0)
    half_col = lax.broadcasted_iota(jnp.int32, (mid, span), 1)
    left = half_col < mid
    upper = low(jnp.where(row <= col, 1.0, 0.0))
    folded = half_col - jnp.where(left, 0, mid)
    eye = jnp.where(half_row == folded, 1.0, 0.0)
    beside = (half_row ^ folded) == 1
    eye_k = jnp.where(
        lax.broadcasted_iota(jnp.int32, (HEAD_DIM, HEAD_DIM), 0)
        == lax.broadcasted_iota(jnp.int32, (HEAD_DIM, HEAD_DIM), 1),
        1.0,
        0.0,
    )
    none = jnp.zeros_like(eye_k)

    units = []
    for i in range(PAIR):
        c = pair * PAIR + i
        tokens = pl.ds(pl.multiple_of(c * span, span), span)
        query_f = q_ref[:, tokens].astype(jnp.float32)
        key_f = k_ref[:, tokens].astype(jnp.float32)
        log_keep = -math.exp(-0.5) / (1.0 + jnp.exp(-d_ref[:, tokens].astype(jnp.float32)))
        squares = (key_f * key_f).reshape(heads, HEAD_DIM, span)
        norm = lax.rsqrt(jnp.sum(squares, axis=1, keepdims=True) + 1e-05)
        unit = (key_f.reshape(heads, HEAD_DIM, span) * norm).reshape(channels, span)
        eraser = unit / (1.0 + jnp.exp(-e_ref[:, tokens].astype(jnp.float32)))

        high = low(log_keep)
        rest = log_keep - high.astype(jnp.float32)
        next_high = low(rest)
        last = low(rest - next_high.astype(jnp.float32))
        cumulative = dot(
            jnp.concatenate([high, next_high], axis=1), jnp.concatenate([upper, upper], axis=0)
        ) + dot(last, upper)
        prior = cumulative - log_keep
        total = cumulative[:, span - 1 :]
        middle = cumulative[:, mid - 1 : mid]
        prior_up = jnp.exp(prior - middle)
        cum_down = jnp.exp(middle - cumulative)
        cum_up = jnp.exp(cumulative - middle)
        prior_down = jnp.exp(middle - prior)
        to_middle = jnp.exp(middle)
        from_middle = jnp.exp(total - middle)
        decay = jnp.exp(total)
        sides = (
            (unit * prior_up, query_f * cum_up, key_f * cum_down, eraser * cum_down, to_middle),
            (unit * cum_down, query_f * prior_down, key_f * prior_up, eraser * prior_up, from_middle),
        )
        for h in range(heads):
            at = slice(h * HEAD_DIM, (h + 1) * HEAD_DIM)
            m = dict(
                c=c, h=h, at=at, tokens=tokens, decay=decay[at],
                scale_out=(from_middle[at], to_middle[at]),
                k=[], e=[], u0=[], q0=[], key_mix=[], key_read=[], erase_read=[],
            )
            mixes = []
            for side, (u, q, k, e, scale_in) in enumerate(sides):
                uq = jnp.concatenate([low(u[at]), low(q[at])], axis=1)
                kb, eb = low(k[at]), low(e[at])
                mk = dot(kb, uq, TN)
                me = dot(eb, uq, TN)
                m["k"].append(kb)
                m["e"].append(eb)
                m["u0"].append(low(u[at] * scale_in[at]))
                m["q0"].append(q[at] * scale_in[at])
                m["key_mix"].append(low(mk[:, :span]) * mask_ref[side])
                m["key_read"].append(low(mk[:, span:]) * mask_ref[2 + side])
                m["erase_read"].append(low(me[:, span:]) * mask_ref[2 + side])
                mixes.append(me[:, :span])
            m["mix"] = low(mixes[0]) * mask_ref[0] + low(mixes[1]) * mask_ref[1]
            ahead, behind = (jnp.where(left, x[:mid], x[mid:]) for x in mixes)
            first = jnp.where(half_row < folded, ahead, behind)
            m["both"] = eye - jnp.where(beside, first, 0.0)
            units.append(m)

    for level in range(1, levels):
        held = [low(m["both"]) for m in units]
        half = [
            low(dot(x * fold_ref[level - 1], m["mix"] * mask_ref[2 + 2 * level]))
            for x, m in zip(held, units)
        ]
        gone = [
            dot(y, jnp.concatenate([x, x], axis=0) * mask_ref[3 + 2 * level])
            for y, x in zip(half, held)
        ]
        if level < levels - 1:
            for m, g in zip(units, gone):
                m["both"] = m["both"] - g
        else:
            for m, x, g in zip(units, held, gone):
                up, down = x * fold_ref[levels - 1], x * fold_ref[levels]
                cross = low(-g)
                zero = jnp.zeros_like(x)
                m["solved"] = (
                    jnp.concatenate([jnp.where(left, up, cross), jnp.where(left, zero, up)], axis=0),
                    jnp.concatenate([jnp.where(left, down, zero), jnp.where(left, cross, down)], axis=0),
                )

    for m in units:
        c, h, at, tokens = m["c"], m["h"], m["at"], m["tokens"]
        v = v_ref[at, tokens]
        vm = low(dot(v, jnp.concatenate(m["key_mix"], axis=1)))
        vr = dot(v, m["key_read"][0] + m["key_read"][1])
        removed = [
            low(dot(jnp.concatenate([vm[:, side * span : (side + 1) * span], m["u0"][side]], axis=0), m["solved"][side]))
            for side in range(2)
        ]
        zero = jnp.zeros((HEAD_DIM, span), jnp.bfloat16)
        reach = [
            jnp.concatenate([removed[0], zero], axis=0),
            jnp.concatenate([removed[1][:HEAD_DIM], zero, removed[1][HEAD_DIM:]], axis=0),
        ]
        taken = dot(jnp.concatenate(reach, axis=1), jnp.concatenate(m["erase_read"], axis=0))
        out_ref[at, tokens] = vr - taken[:HEAD_DIM]
        added = dot(jnp.concatenate(m["k"], axis=0), v, NT)
        for side in range(2):
            near = slice((1 + side) * HEAD_DIM, (2 + side) * HEAD_DIM)
            read_ref[side, at, tokens] = low(m["q0"][side] - taken[near])
            gone = dot(m["e"][side], removed[side], NT)
            scale = m["scale_out"][side]
            state = (added[side * HEAD_DIM : (side + 1) * HEAD_DIM] - gone[:, :HEAD_DIM]) * scale
            moved = eye_k * m["decay"] - gone[:, HEAD_DIM:] * scale
            step_ref[c, side, h] = jnp.concatenate([state, moved], axis=1)

    for i in range(PAIR):
        c = pair * PAIR + i
        for h in range(heads):
            step = step_ref[c, 0, h]
            new = close_dot(step[:, HEAD_DIM:], map_ref[0, h])
            map_ref[0, h] = new + jnp.concatenate([step[:, :HEAD_DIM], none], axis=1)
            before = map_ref[1, h]
            new = close_dot(before[:, HEAD_DIM:], step_ref[c, 1, h])
            map_ref[1, h] = new + jnp.concatenate([before[:, :HEAD_DIM], none], axis=1)


def layer_kernel(
    ep_count, tp_count, capacity,
    gate_hbm, up_hbm, down_hbm,
    input_hbm, scale_hbm, routes_hbm, weights_hbm, q_hbm, k_hbm, v_hbm, e_hbm, d_hbm, gain_hbm,
    out_ref, result_ref,
    gate_ref, up_ref, down_ref,
    input_ref, scale_ref, routes_ref, weights_ref, q_ref, k_ref, v_ref, e_ref, d_ref, gain_ref,
    arrived_ref, comb_ref, read_ref, local_ref, step_ref, maps_ref,
    map_ref, mask_ref, fold_ref, normed_ref, pick_ref, quarter_ref, near_ref, far_ref,
    hidden_ref, part_ref, sum_ref, column_ref,
    relay_ref, total_ref, peers_ref, returned_ref, gathered_ref, enter_ref, states_ref,
    load_sem, send_a, recv_a, send_s, recv_s, send_f, recv_f, send_m, recv_m,
    send_t, recv_t, send_r, recv_r, send_z, recv_z,
):
    loads = [
        pltpu.make_async_copy(a, b, load_sem.at[i])
        for i, (a, b) in enumerate(
            (
                (input_hbm, input_ref), (scale_hbm, scale_ref), (routes_hbm, routes_ref),
                (weights_hbm, weights_ref), (gain_hbm, gain_ref),
                (q_hbm, q_ref), (k_hbm, k_ref), (v_hbm, v_ref), (e_hbm, e_ref), (d_hbm, d_ref),
                (gate_hbm, gate_ref), (up_hbm, up_ref), (down_hbm, down_ref),
            )
        )
    ]
    for load in loads:
        load.start()
    mine, column = lax.axis_index("ep"), lax.axis_index("tp")
    rounds = q_ref.shape[1] // (SPAN * PAIR)
    count, features = input_ref.shape
    width = features // tp_count
    units = gate_ref.shape[1]
    blocks, _, heads = step_ref.shape[:3]
    groups = min(GROUPS, ep_count)
    per = ep_count // groups
    last = tp_count - 1
    part = own = pl.ds(pl.multiple_of(column * width, width), width)
    facing = pl.ds(pl.multiple_of(flipped(column, last) * width, width), width)
    met = greet(ep_count, tp_count, mine, column)
    for load in loads[:5]:
        load.wait()

    def normalize(i, carry):
        rows = pl.ds(pl.multiple_of(i * ROWS, ROWS), ROWS)
        x = input_ref[rows, :].astype(jnp.float32)
        mean = jnp.mean(x * x, axis=-1, keepdims=True)
        normed_ref[rows, :] = low(x * lax.rsqrt(mean + 1e-06) * scale_ref[...])
        return carry

    lax.fori_loop(0, count // ROWS, normalize, 0)

    names = lax.broadcasted_iota(jnp.int32, (ep_count, count), 0)
    chosen = jnp.zeros((ep_count, count), jnp.float32)
    weight = jnp.zeros((ep_count, count), jnp.float32)
    for k in range(routes_ref.shape[0]):
        named = jnp.where(names == routes_ref[k : k + 1, :], 1.0, 0.0)
        chosen = chosen + named
        weight = weight + named * weights_ref[k : k + 1, :]
    earlier = lax.broadcasted_iota(jnp.int32, (count, count), 0)
    later = lax.broadcasted_iota(jnp.int32, (count, count), 1)
    before = dot(low(chosen), low(jnp.where(earlier < later, 1.0, 0.0)))
    place = jnp.where(chosen > 0.5, before, -1.0)
    slots = lax.broadcasted_iota(jnp.int32, (capacity, count), 0).astype(jnp.float32)
    for e in range(ep_count):
        pick_ref[e] = low(jnp.where(slots == place[e : e + 1, :], 1.0, 0.0))

    mine_part = normed_ref[:, part]
    if capacity % 16 == 0:
        picks = pick_ref[...].reshape(ep_count * capacity, count)
        quarter_ref[...] = low(dot(picks, mine_part)).reshape(ep_count, capacity, width)
    else:
        for e in range(ep_count):
            quarter_ref[e] = low(dot(pick_ref[e], mine_part))
    for r in range(per):
        rows = low(dot(pick_ref[flipped(mine, r)], normed_ref[...]))
        if r:
            near_ref[r] = rows
        else:
            arrived_ref[mine] = rows
    away, extra = {}, {}
    for s in range(1, ep_count):
        target = flipped(mine, s)
        ends = (send_a.at[0, s], recv_a.at[0, s])
        if s < per:
            away[s] = remote("ep", target, near_ref.at[s], arrived_ref.at[mine], *ends)
        else:
            away[s] = remote(
                "ep", target, quarter_ref.at[target], arrived_ref.at[mine, :, part], *ends
            )
    met()
    for s in range(per, ep_count):
        away[s].start()
    for r in range(per if groups > 1 else 0):
        far_ref[r] = low(dot(pick_ref[flipped(mine, per + r)], normed_ref[:, facing]))
    for s in range(1, per):
        away[s].start()
    write_masks(mask_ref, fold_ref)
    for s in range(per, min(2 * per, ep_count)):
        extra[s] = remote(
            "ep", flipped(mine, s), far_ref.at[s - per], arrived_ref.at[mine, :, facing],
            send_a.at[1, s], recv_a.at[1, s],
        )
        extra[s].start()

    square = tp_count == 4 and per % 2 == 0
    spread, onward = {}, {}
    for k in range(1, groups):
        first = flipped(lax.div(mine, per), k) * per
        block = arrived_ref.at[pl.ds(first, per), :, part]
        for p in range(1, last if k == 1 or square else tp_count):
            spread[k, p] = remote(
                "tp", flipped(column, p), block, block, send_s.at[k, p], recv_s.at[k, p]
            )
        for route in range(2 if square and k > 1 else 0):
            came = pl.ds(pl.multiple_of(flipped(column, 1 + route) * width, width), width)
            block = arrived_ref.at[pl.ds(first + route * (per // 2), per // 2), :, came]
            onward[k, route] = remote(
                "tp", flipped(column, 2 - route), block, block,
                send_f.at[k, route], recv_f.at[k, route],
            )

    def pass_on(k):
        for s in range(k * per, (k + 1) * per):
            away[s].wait_recv()
        for (group, _), copy in spread.items():
            if group == k:
                copy.start()

    def forward(k):
        for route in range(2 if square else 0):
            spread[k, 1 + route].wait_recv()
            onward[k, route].start()

    def complete(k):
        if k == 0:
            for s in range(1, per):
                away[s].wait_recv()
        for (group, _), copy in (onward if square and k > 1 else spread).items():
            if group == k:
                copy.wait_recv()
        for s, copy in extra.items():
            if s // per == k:
                copy.wait_recv()

    for h in range(map_ref.shape[1]):
        start = jnp.concatenate(
            [
                jnp.zeros((HEAD_DIM, HEAD_DIM), jnp.float32),
                jnp.where(
                    lax.broadcasted_iota(jnp.int32, (HEAD_DIM, HEAD_DIM), 0)
                    == lax.broadcasted_iota(jnp.int32, (HEAD_DIM, HEAD_DIM), 1),
                    1.0,
                    0.0,
                ),
            ],
            axis=1,
        )
        map_ref[0, h] = start
        map_ref[1, h] = start
    for e in range(ep_count):
        share = pick_ref[e].astype(jnp.float32) * weight[e : e + 1, :]
        high, rest = split(share)
        comb_ref[0, e] = high
        comb_ref[1, e] = rest

    for h in range(heads):
        lanes = min(2 * HEAD_DIM, heads * HEAD_DIM)
        at = h * HEAD_DIM // lanes * lanes
        row = lax.broadcasted_iota(jnp.int32, (HEAD_DIM, lanes), 0)
        lane = lax.broadcasted_iota(jnp.int32, (HEAD_DIM, lanes), 1)
        picked = jnp.where(lane == row + (h * HEAD_DIM - at), gain_ref[:, at : at + lanes], 0.0)
        column_ref[h * HEAD_DIM : (h + 1) * HEAD_DIM, :] = jnp.sum(picked, axis=1, keepdims=True)

    sides = {}
    for s in range(1, ep_count):
        target = lax.rem(mine + s, ep_count)
        sides[s] = remote(
            "ep", target, maps_ref.at[lax.div(mine + s, ep_count)], gathered_ref.at[mine],
            send_m.at[s], recv_m.at[s],
        )

    def quarter(index):
        return pl.ds(pl.multiple_of(index * width, width), width)

    def shares(k):
        first = flipped(lax.div(mine, per), k) * per
        if not square:
            rows = pl.ds(first, per)
            return [
                remote(
                    "tp", flipped(column, p),
                    part_ref.at[rows, :, quarter(flipped(column, p))],
                    peers_ref.at[p - 1, rows],
                    send_t.at[k, p - 1], recv_t.at[k, p - 1],
                )
                for p in range(1, tp_count)
            ]
        made = []
        for route in range(2):
            rows = pl.ds(first + route * (per // 2), per // 2)
            for i, want in ((1, last), (0, 1 + route)):
                made.append(
                    remote(
                        "tp", flipped(column, 1 + route),
                        part_ref.at[rows, :, quarter(flipped(column, want))],
                        peers_ref.at[i, rows],
                        send_t.at[k, 2 * route + i], recv_t.at[k, 2 * route + i],
                    )
                )
        return made

    def onto(k, route):
        first = flipped(lax.div(mine, per), k) * per
        rows = pl.ds(first + route * (per // 2), per // 2)
        return remote(
            "tp", flipped(column, 2 - route), relay_ref.at[rows], peers_ref.at[2, rows],
            send_r.at[k, route], recv_r.at[k, route],
        )

    def relay(k):
        if not square:
            return
        first = flipped(lax.div(mine, per), k) * per
        copies = shares(k)
        for route in range(2):
            copies[2 * route].wait_recv()
            for r in range(route * (per // 2), (route + 1) * (per // 2)):
                share = part_ref[first + r, :, quarter(flipped(column, 2 - route))]
                relay_ref[first + r] = low(
                    share.astype(jnp.float32) + peers_ref[1, first + r].astype(jnp.float32)
                )
            onto(k, route).start()

    def back(s):
        target = flipped(mine, s)
        return pltpu.make_async_remote_copy(
            src_ref=total_ref.at[target],
            dst_ref=returned_ref.at[mine],
            send_sem=send_z.at[s],
            recv_sem=recv_z.at[s],
            device_id={"ep": target},
            device_id_type=MESH,
        )

    def product(k):
        first = flipped(lax.div(mine, per), k) * per
        joined = capacity % 16 == 0
        for r in range(1 if joined else per):
            at = pl.ds(first + r, per if joined else 1)
            count = at.size * capacity
            x = arrived_ref[at].reshape(count, features)
            for lo in range(0, units, 128):
                hi = min(units, lo + 128)
                if hi - lo == 128:
                    both = dot(
                        x, jnp.concatenate([gate_ref[:, lo:hi], up_ref[:, lo:hi]], axis=1)
                    )
                    gate, up = both[:, :128], both[:, 128:]
                else:
                    gate, up = dot(x, gate_ref[:, lo:hi]), dot(x, up_ref[:, lo:hi])
                hidden_ref[:count, lo:hi] = low(gate / (1.0 + jnp.exp(-gate)) * up)
            hidden = hidden_ref[:count, :]
            for lo in range(0, features, 256):
                made = low(dot(hidden, down_ref[:, lo : lo + 256]))
                part_ref[at, :, lo : lo + 256] = made.reshape(at.size, capacity, 256)

    def give_back(k):
        first = flipped(lax.div(mine, per), k) * per
        if square:
            copies = shares(k)
            for route in range(2):
                copies[2 * route + 1].wait_recv()
                onto(k, route).wait_recv()
        else:
            for copy in shares(k):
                copy.wait_recv()
        for r in range(per):
            total = part_ref[first + r, :, own].astype(jnp.float32)
            for p in (0, 2) if square else range(tp_count - 1):
                total = total + peers_ref[p, first + r].astype(jnp.float32)
            total_ref[first + r] = low(total)
        for s in range(k * per, (k + 1) * per):
            if s:
                back(s).start()
            else:
                returned_ref[mine] = total_ref[mine]

    def gather(j, carry):
        for side, at in ((0, j), (1, ep_count - 1 - j)):
            reached = at < mine if side == 0 else at > mine

            @pl.when(reached)
            def _():
                for h in range(heads):
                    part = gathered_ref[at, h]
                    high, rest = split(enter_ref[side, h])
                    new = dot(part[:, HEAD_DIM:], jnp.concatenate([high, rest], axis=1))
                    enter_ref[side, h] = (
                        new[:, :HEAD_DIM] + new[:, HEAD_DIM:] + part[:, :HEAD_DIM].astype(jnp.float32)
                    )

        return carry

    def chain(j, carry):
        for side, at in ((0, j), (1, blocks - 1 - j)):
            for h in range(heads):
                step = step_ref[at, side, h]
                state = enter_ref[side, h]
                states_ref[at, h, side * HEAD_DIM : (side + 1) * HEAD_DIM, :] = low(state)
                enter_ref[side, h] = step[:, :HEAD_DIM] + close_dot(step[:, HEAD_DIM:], state)
        return carry

    def write(j, carry):
        tokens = pl.ds(pl.multiple_of(j * SPAN, SPAN), SPAN)
        for h in range(heads):
            at = slice(h * HEAD_DIM, (h + 1) * HEAD_DIM)
            reads = jnp.concatenate([read_ref[0, at, tokens], read_ref[1, at, tokens]], axis=0)
            summed = local_ref[at, tokens] + dot(states_ref[j, h], reads, TN)
            center = jnp.mean(summed, axis=0, keepdims=True)
            moved = summed - center
            spread = jnp.mean(moved * moved, axis=0, keepdims=True)
            scaled = moved * lax.rsqrt(spread + HEAD_DIM * 1e-05) * column_ref[at, :]
            out_ref[at, tokens] = low(scaled)
        return carry

    enter_ref[...] = jnp.zeros_like(enter_ref)
    for load in loads[5:]:
        load.wait()
    def enter_states():
        for s in range(1, ep_count):
            sides[s].wait_recv()
        lax.fori_loop(0, ep_count, gather, 0)
        lax.fori_loop(0, blocks, chain, 0)

    def send_maps():
        maps_ref[...] = low(map_ref[...])
        for s in range(1, ep_count):
            sides[s].start()

    def scatter(k):
        for copy in shares(k):
            copy.start()

    acts = {
        "c": complete,
        "P": pass_on,
        "F": forward,
        "S": scatter,
        "R": relay,
        "B": give_back,
        "M": lambda _: send_maps(),
        "E": lambda _: enter_states(),
        "W": lambda i: lax.fori_loop(blocks * i // 2, blocks * (i + 1) // 2, write, 0),
    }
    if (groups, rounds) == (4, 4):
        plan = PLAN
    else:
        plan = ["c0", "p0", "S0"]
        for k in range(1, groups):
            plan += [f"P{k}", f"F{k}"] if k > 1 else ["P1"]
            plan += [f"c{k}", f"p{k}", f"S{k}"]
        plan += [f"m{c}" for c in range(rounds)] + ["M0", "E0"]
        plan += [f"R{k}" for k in range(groups)] + ["W0", "W1"]
        plan += [f"B{k}" for k in range(groups)]
    steps, ahead = [], []
    for word in plan:
        kind, index = word[0], int(word[1:])
        if kind in "pm":
            steps.append((ahead, kind, index))
            ahead = []
        else:
            ahead.append((kind, index))

    def work(i, carry):
        group, block = jnp.int32(0), jnp.int32(0)
        multiplies = i < 0
        for at, (before, kind, index) in enumerate(steps):
            if kind == "p":
                group = jnp.where(i == at, index, group)
                multiplies = jnp.logical_or(multiplies, i == at)
            else:
                block = jnp.where(i == at, index, block)
            if before:

                @pl.when(i == at)
                def _():
                    for act, k in before:
                        acts[act](k)

        @pl.when(multiplies)
        def _():
            product(group)

        @pl.when(jnp.logical_not(multiplies))
        def _():
            local_block(
                block, q_ref, k_ref, v_ref, e_ref, d_ref,
                read_ref, local_ref, step_ref, map_ref, mask_ref, fold_ref,
            )

        return carry

    lax.fori_loop(0, len(steps), work, 0)
    for act, k in ahead:
        acts[act](k)
    order = [int(word[1:]) for word in plan if word[0] == "B"]

    for k in order:
        for s in range(max(1, k * per), (k + 1) * per):
            back(s).wait_recv()
        first = flipped(lax.div(mine, per), k) * per
        for i in range(2):
            if capacity % 16 == 0:
                at = pl.ds(first, per)
                made = dot(
                    comb_ref[i, at].reshape(per * capacity, -1),
                    returned_ref[at].reshape(per * capacity, width),
                    TN,
                )
            else:
                made = dot(comb_ref[i, first], returned_ref[first], TN)
                for r in range(1, per):
                    made = made + dot(comb_ref[i, first + r], returned_ref[first + r], TN)
            if k == order[0] and i == 0:
                sum_ref[...] = made
            else:
                sum_ref[...] = sum_ref[...] + made
    result_ref[...] = low(sum_ref[...])
    for s in range(1, ep_count):
        away[s].wait_send()
        back(s).wait_send()
        sides[s].wait_send()
    for copy in (*extra.values(), *spread.values(), *onward.values()):
        copy.wait_send()
    for k in range(groups):
        for copy in shares(k):
            copy.wait_send()
        for route in range(2 if square else 0):
            onto(k, route).wait_send()


def layer(
    gate, up, down, expert_in, expert_gain, routes, route_weight,
    query_in, key_in, value_in, erase_pre, decay_pre, mix_gain,
):
    channels, seq_len = query_in.shape
    count, features = expert_in.shape
    ep_count, tp_count = lax.axis_size("ep"), lax.axis_size("tp")
    capacity = 3 * routes.shape[1] * count // (2 * ep_count)
    width = features // tp_count
    units = gate.shape[1]
    heads = channels // HEAD_DIM
    blocks = seq_len // SPAN
    groups = min(GROUPS, ep_count)
    per = ep_count // groups
    levels = level_count()
    f32, bf16 = jnp.float32, jnp.bfloat16
    whole = pl.BlockSpec(memory_space=pltpu.VMEM)
    stays = pl.BlockSpec(memory_space=pltpu.HBM)
    dma = pltpu.SemaphoreType.DMA
    scratch = [
        (gate.shape, bf16),
        (up.shape, bf16),
        (down.shape, bf16),
        (expert_in.shape, bf16),
        ((1, features), f32),
        (routes.T.shape, routes.dtype),
        (routes.T.shape, f32),
        *[((channels, seq_len), bf16)] * 5,
        ((1, channels), f32),
        ((ep_count, capacity, features), bf16),
        ((2, ep_count, capacity, count), bf16),
        ((2, channels, seq_len), bf16),
        ((channels, seq_len), f32),
        ((blocks, 2, heads, HEAD_DIM, 2 * HEAD_DIM), f32),
        ((2, heads, HEAD_DIM, 2 * HEAD_DIM), bf16),
        ((2, heads, HEAD_DIM, 2 * HEAD_DIM), f32),
        ((2 + 2 * levels, SPAN, SPAN), bf16),
        ((levels + 1, SPAN // 2, SPAN), bf16),
        ((count, features), bf16),
        ((ep_count, capacity, count), bf16),
        ((ep_count, capacity, width), bf16),
        ((per, capacity, features), bf16),
        ((per, capacity, width), bf16),
        ((per * capacity, units), bf16),
        ((ep_count, capacity, features), bf16),
        ((count, width), f32),
        ((channels, 1), f32),
        ((ep_count, capacity, width), bf16),
        ((ep_count, capacity, width), bf16),
        ((max(3, tp_count - 1), ep_count, capacity, width), bf16),
        ((ep_count, capacity, width), bf16),
        ((ep_count, heads, HEAD_DIM, 2 * HEAD_DIM), bf16),
        ((2, heads, HEAD_DIM, HEAD_DIM), f32),
        ((blocks, heads, 2 * HEAD_DIM, HEAD_DIM), bf16),
    ]
    return pl.pallas_call(
        functools.partial(layer_kernel, ep_count, tp_count, capacity),
        in_specs=[stays] * 13,
        out_specs=[whole] * 2,
        out_shape=[
            jax.ShapeDtypeStruct((channels, seq_len), bf16),
            jax.ShapeDtypeStruct((count, width), bf16),
        ],
        scratch_shapes=[pltpu.VMEM(*one) for one in scratch]
        + [
            dma((13,)),
            dma((2, ep_count)),
            dma((2, ep_count)),
            dma((groups, tp_count)),
            dma((groups, tp_count)),
            dma((groups, 2)),
            dma((groups, 2)),
            dma((ep_count,)),
            dma((ep_count,)),
            dma((groups, max(4, tp_count))),
            dma((groups, max(4, tp_count))),
            dma((groups, 2)),
            dma((groups, 2)),
            dma((ep_count,)),
            dma((ep_count,)),
        ],
        compiler_params=pltpu.CompilerParams(
            collective_id=0, has_side_effects=True, vmem_limit_bytes=53 << 20
        ),
        cost_estimate=pl.CostEstimate(
            flops=int(6e10 * heads * blocks / 32), bytes_accessed=1 << 24, transcendentals=1 << 20
        ),
        name="layer",
    )(
        gate, up, down, expert_in, expert_gain.reshape(1, features), routes.T, route_weight.T,
        query_in, key_in, value_in, erase_pre, decay_pre, mix_gain.reshape(1, channels),
    )


def on_device(
    query_in,
    key_in,
    value_in,
    erase_pre,
    decay_pre,
    mix_gain,
    expert_in,
    expert_gain,
    routes,
    route_weight,
    gate_weight,
    up_weight,
    down_weight,
):
    return layer(
        gate_weight.reshape(gate_weight.shape[1:]),
        up_weight.reshape(up_weight.shape[1:]),
        down_weight.reshape(down_weight.shape[1:]),
        expert_in, expert_gain, routes, route_weight,
        query_in, key_in, value_in, erase_pre, decay_pre, mix_gain,
    )


def solution(mesh):
    placed = (
        P("tp", "ep"),
        P("tp", "ep"),
        P("tp", "ep"),
        P("tp", "ep"),
        P("tp", "ep"),
        P("tp"),
        P("ep", None),
        P(),
        P("ep", None),
        P("ep", None),
        P("ep", None, "tp"),
        P("ep", None, "tp"),
        P("ep", "tp", None),
    )
    return jax.shard_map(
        on_device,
        mesh=mesh,
        in_specs=placed,
        out_specs=(P("tp", "ep"), P("ep", "tp")),
        check_vma=False,
    )
```
